32 devices in a mesh: row: 16 (over z, y, x), col: 2 (over core).
Axes of the slice: x: 2, y: 2, z: 4, core: 2. Of those that a mesh axis runs over, the one named last changes fastest.
Arguments:
- tokens: bfloat16 [2, 8192, 2048], P(None, 'row'), may hold values from -6 to 6
- w_value: bfloat16 [2048, 1024], P(None, 'col'), may hold values from -0.125 to 0.125
- w_first: bfloat16 [2048, 1024], P(None, 'col'), may hold values from -0.125 to 0.125
- w_second: bfloat16 [2048, 1024], P(None, 'col'), may hold values from -0.125 to 0.125
- short_taps: float32 [3, 3, 1024], P(None, None, 'col'), may hold values from -3.5 to 3.5
- filter_in: float32 [33, 64], replicated, may hold values from -2 to 2
- filter_mid: float32 [64, 64], replicated, may hold values from -1.5 to 1.5
- filter_out: float32 [64, 2, 2, 1024], P(None, None, None, 'col'), may hold values from -0.75 to 0.75
- decay_rate: float32 [1024], P('col'), may hold values from 0 to 1, as said below
- skip_gain: float32 [2, 1024], P(None, 'col'), may hold values from -4 to 4
- w_output: bfloat16 [1024, 2048], P(None, 'col'), may hold values from -0.1875 to 0.1875
Outputs:
- mixed_out: bfloat16 [2, 8192, 2048], P(None, 'row', 'col')
The draws below stay inside these ranges and needn't reach their ends.
Inputs may be any that keep to these rules, and one draw needn't show every extreme that they name: `decay_rate`: Per-position decay rates of the channels' filters; all positive.
All inputs are finite; a program needn't handle non-finite values.
Results may differ from the reference program's by a relative error of at most 0.007.
Values may be sent and summed in bfloat16 or wider, within the bound.
A program may use at most 128 MiB of HBM per device.

```python
import math
import jax
import jax.numpy as jnp
from jax import lax

WIDTH = 2048
CHANNELS = 1024
FEATS = 33
FILTER_UNITS = 64
SEQS = 2
LENGTH = 8192


def draw_decay_rate(key, part):
    base = jax.random.fold_in(key, 71)
    pick_key, slow_key, fast_key = jax.random.split(base, 3)
    slow_share = 0.5
    chooser = jax.random.uniform(pick_key, (CHANNELS,), jnp.float32)
    slow_log = jax.random.uniform(slow_key, (CHANNELS,), jnp.float32, jnp.log(0.05 / LENGTH), jnp.log(2.0 / LENGTH))
    fast_log = jax.random.uniform(fast_key, (CHANNELS,), jnp.float32, jnp.log(1.0 / 100.0), jnp.log(1.0 / 30.0))
    return jnp.where(chooser < slow_share, jnp.exp(slow_log), jnp.exp(fast_log)).astype(jnp.float32)


def shard_levels(key, shape, cuts, low, high):
    factor_of = 1.0
    for position, blocks in cuts:
        heights = jax.random.uniform(jax.random.fold_in(jax.random.fold_in(key, 6), position), (blocks,), jnp.float32, low / len(cuts), high / len(cuts))
        factor_of = factor_of * jnp.repeat(jnp.exp(heights), shape[position] // blocks).reshape((-1,) + (1,) * (len(shape) - 1 - position))
    return factor_of


def scatter_about(own_key, dims, scale, reach, cuts=(), kind=jnp.bfloat16):
    gain = shard_levels(own_key, dims, cuts, -0.22, 0.18) if cuts else 1.0
    result = jax.random.normal(own_key, dims, jnp.float32) * scale * gain
    return jnp.minimum(jnp.maximum(result, -reach), reach).astype(kind)


def setup_inputs(seed: int = 0) -> dict:
    key_of = jax.random.split(jax.random.key(seed), 12)
    return {
        "tokens": scatter_about(key_of[0], (SEQS, LENGTH, WIDTH), 1.0, 6.0, ((1, 16),)),
        "w_value": scatter_about(key_of[1], (WIDTH, CHANNELS), WIDTH ** -0.5, 0.125, ((1, 2),)),
        "w_first": scatter_about(key_of[2], (WIDTH, CHANNELS), WIDTH ** -0.5, 0.125, ((1, 2),)),
        "w_second": scatter_about(key_of[3], (WIDTH, CHANNELS), WIDTH ** -0.5, 0.125, ((1, 2),)),
        "short_taps": scatter_about(key_of[4], (3, 3, CHANNELS), 3 ** -0.5, 3.5, ((2, 2),), jnp.float32),
        "filter_in": jnp.clip(jax.random.uniform(key_of[5], (FEATS, FILTER_UNITS), jnp.float32, -2.0, 2.0), -2.0, 2.0),
        "filter_mid": jnp.clip(jax.random.uniform(key_of[6], (FILTER_UNITS, FILTER_UNITS), jnp.float32, -1.5, 1.5), -1.5, 1.5),
        "filter_out": scatter_about(key_of[7], (FILTER_UNITS, 2, 2, CHANNELS), FILTER_UNITS ** -0.5, 0.75, ((3, 2),), jnp.float32),
        "decay_rate": draw_decay_rate(jax.random.fold_in(key_of[11], 71), 0),
        "skip_gain": scatter_about(key_of[9], (2, CHANNELS), 1.0, 4.0, ((1, 2),), jnp.float32),
        "w_output": scatter_about(key_of[10], (CHANNELS, WIDTH), CHANNELS ** -0.5, 0.1875, ((1, 2),)),
    }


def position_features(length, band_count):
    lag_index = jnp.arange(length, dtype=jnp.float32)
    ramp_line = lag_index / (length - 1)
    omega_step = 2.0 * math.pi / length * lag_index
    band_freq = jnp.linspace(0.0001, band_count - 1, band_count, dtype=jnp.float32)
    angle = omega_step[:, None] * band_freq[None, :]
    return jnp.concatenate([ramp_line[:, None], jnp.cos(angle), -jnp.sin(angle)], axis=1)

def make_kernel(hidden, out_block, rate_block, length):
    shaped = jnp.einsum('lh,hsoc->solc', hidden, out_block, precision=lax.Precision.HIGHEST)
    lag_index = jnp.arange(length, dtype=jnp.float32)
    shaped = shaped * jnp.exp(-lag_index[:, None] * rate_block[None, :])
    ahead_half = shaped[0]
    behind_half = shaped[1]
    zero_col = jnp.zeros((2, 1, ahead_half.shape[2]), jnp.float32)
    kernel = jnp.concatenate([ahead_half, zero_col, behind_half[:, 1:][:, ::-1]], axis=1)
    return kernel * lax.rsqrt(lax.optimization_barrier(jnp.sum(kernel * kernel, axis=1, keepdims=True)) + 1e-06)

def one_sequence(tokens, w_value, w_first, w_second, short_taps, filter_in, filter_mid, filter_out, decay_rate, skip_gain, w_output):
    length = tokens.shape[0]
    channel_count = w_value.shape[1]
    stacked = jnp.stack([jnp.dot(tokens, weight, preferred_element_type=jnp.float32).astype(jnp.bfloat16) for weight in (w_value, w_first, w_second)])
    stacked = lax.optimization_barrier(stacked).astype(jnp.float32)
    padded = jnp.pad(stacked, ((0, 0), (1, 1), (0, 0)))
    smoothed = short_taps[0][:, None, :] * padded[:, :length] + short_taps[1][:, None, :] * padded[:, 1:length + 1] + short_taps[2][:, None, :] * padded[:, 2:]
    band_count = (filter_in.shape[0] - 1) // 2
    features = position_features(length, band_count)
    hidden = jnp.sin(jnp.dot(features, filter_in, precision=lax.Precision.HIGHEST))
    hidden = jnp.sin(jnp.dot(hidden, filter_mid, precision=lax.Precision.HIGHEST))
    block_count = channel_count // 128
    blocks_in = smoothed.reshape(3, length, block_count, 128).transpose(2, 0, 1, 3)
    out_blocks = filter_out.reshape(filter_out.shape[0], 2, 2, block_count, 128).transpose(3, 0, 1, 2, 4)
    rate_blocks = decay_rate.reshape(block_count, 128)
    gain_blocks = skip_gain.reshape(2, block_count, 128).transpose(1, 0, 2)

    def one_block(packed):
        parts, out_block, rate_block, gain_block = packed
        kernel = make_kernel(hidden, out_block, rate_block, length)
        spectrum = jnp.fft.rfft(kernel, axis=1)
        carried = parts[0]
        for order_idx in range(2):
            state_spec = jnp.fft.rfft(carried, n=2 * length, axis=0)
            reach_term = jnp.fft.irfft(state_spec * spectrum[order_idx], n=2 * length, axis=0)[:length]
            carried = parts[order_idx + 1] * (reach_term + gain_block[order_idx][None, :] * carried)
        return carried.astype(jnp.bfloat16)
    gated_blocks = lax.map(one_block, (blocks_in, out_blocks, rate_blocks, gain_blocks))
    gated_out = gated_blocks.transpose(1, 0, 2).reshape(length, channel_count)
    return jnp.dot(gated_out, w_output, preferred_element_type=jnp.float32).astype(jnp.bfloat16)

def reference(tokens, w_value, w_first, w_second, short_taps, filter_in, filter_mid, filter_out, decay_rate, skip_gain, w_output):

    def run_one(sequence):
        return one_sequence(sequence, w_value, w_first, w_second, short_taps, filter_in, filter_mid, filter_out, decay_rate, skip_gain, w_output)
    return lax.map(run_one, tokens)
```

```python
import functools
import math

import jax
import jax.numpy as jnp
import numpy as np
from jax import lax
from jax.experimental import pallas as pl
from jax.experimental.pallas import tpu as pltpu
from jax.sharding import PartitionSpec as P

LANES = 128
f32 = jnp.float32
bf16 = jnp.bfloat16
highest = lax.Precision.HIGHEST


def split_table(table):
    table = np.asarray(table, np.float32)
    high = table.astype(bf16)
    low = (table - high.astype(np.float32)).astype(bf16)
    return np.stack([high, low])


def transform_tables(full_length):
    rows = full_length // LANES
    half = rows // 2
    r = np.arange(rows)
    q = np.arange(LANES)
    angle_rows = 2.0 * np.pi * ((r[:, None] * r[None, :]) % rows) / rows
    angle_cols = 2.0 * np.pi * ((q[:, None] * q[None, :]) % LANES) / LANES
    angle_turn = 2.0 * np.pi * ((r[:, None] * q[None, :]) % full_length) / full_length
    c1, s1 = np.cos(angle_rows), np.sin(angle_rows)
    c2, s2 = np.cos(angle_cols), np.sin(angle_cols)
    real_rows = split_table(np.concatenate([c1, -s1], 0))
    pair_rows = np.block([[c1[:, :half], s1[:, :half]], [-s1[:, :half], c1[:, :half]]])
    fore_cols = np.block([[c2, -s2], [s2, c2]])
    back_cols = np.block([[c2, s2], [-s2, c2]])
    turn = np.stack([np.cos(angle_turn), np.sin(angle_turn)]).astype(np.float32)
    return (
        real_rows,
        split_table(pair_rows),
        split_table(pair_rows.T),
        split_table(fore_cols),
        split_table(back_cols),
        turn,
    )


def dot(a, b):
    return jnp.dot(a, b, preferred_element_type=f32)


def wave(x):
    turns = jnp.floor(x * (1.0 / math.pi) + 0.5)
    r = x - turns * 3.140625
    r = r - turns * 9.67502593994140625e-4
    r = r - turns * 1.509957990978376e-7
    odd = turns - 2.0 * jnp.floor(turns * 0.5)
    r = r * (1.0 - 2.0 * odd)
    q = r * r
    p = -2.5052108e-8
    for coef in (2.7557319e-6, -1.9841270e-4, 8.3333333e-3, -1.6666667e-1):
        p = p * q + coef
    return r + r * q * p


def filter_kernel(
    bands, length, sig_batch, chunk, steps, w_in, w_mid, w_out, rates, rows_ref, cols_ref, turn_ref,
    spec_ref, line_ref, power_ref
):
    i = pl.program_id(0)
    sigs = w_out.shape[1]
    full = 2 * length
    n1_count = full // LANES

    @pl.when(i == 0)
    def _():
        power_ref[...] = jnp.zeros_like(power_ref)

    @pl.when(i < steps)
    def _():
        feat_rows = w_in.shape[1]
        n = i * chunk + lax.broadcasted_iota(jnp.int32, (1, chunk), 1)
        m = jnp.where(n < length, n, full - n).astype(f32)
        row = lax.broadcasted_iota(jnp.int32, (feat_rows, 1), 0)
        band = jnp.where(row <= bands, row - 1, row - 1 - bands).astype(f32)
        freq = 0.0001 + (bands - 1 - 0.0001) / (bands - 1) * band
        phase = jnp.where(row <= bands, 0.5 * math.pi, math.pi).astype(f32)
        angle = (2.0 * math.pi / length * m) * freq + phase
        feats = jnp.where(
            row == 0, m * (1.0 / (length - 1)), jnp.where(row <= 2 * bands, wave(angle), 0.0)
        )
        hidden = wave(jnp.dot(w_in[...], feats, precision=highest, preferred_element_type=f32))
        hidden = wave(jnp.dot(w_mid[...], hidden, precision=highest, preferred_element_type=f32))
        side = i // (steps // 2)
        shaped = jnp.dot(w_out[side], hidden, precision=highest, preferred_element_type=f32)
        damp = jnp.exp(-rates[:, 0:1] * m)
        damp = jnp.where(n == length, 0.0, damp)
        shaped = shaped * jnp.concatenate([damp, damp], axis=0)
        power = power_ref[...]
        for j in range(chunk // LANES):
            tile = shaped[:, j * LANES : (j + 1) * LANES]
            power = power + tile * tile
            at = pl.multiple_of((i * (chunk // LANES) + j) * sigs, sigs)
            line_ref[pl.ds(at, sigs), :] = tile
        power_ref[...] = power

    @pl.when(i == steps)
    def _():
        total = jnp.sum(power_ref[...], axis=1, keepdims=True)
        power_ref[...] = jnp.broadcast_to(lax.rsqrt(total + 1e-6) * (1.0 / full), power_ref.shape)

    @pl.when(i >= steps)
    def _():
        c, s = turn_ref[0], turn_ref[1]
        first = (i - steps) * sig_batch
        parts = []
        for b in range(sig_batch):
            line = line_ref[pl.ds(first + b, n1_count, stride=sigs), :]
            parts.append(line * power_ref[pl.ds(first + b, 1), :])
        x = jnp.concatenate(parts, axis=1)
        hi = x.astype(bf16)
        lo = (x - hi.astype(f32)).astype(bf16)
        a = dot(rows_ref[0], hi) + dot(rows_ref[1], hi) + dot(rows_ref[0], lo)
        turned = []
        for b in range(sig_batch):
            ar = a[:n1_count, b * LANES : (b + 1) * LANES]
            ai = a[n1_count:, b * LANES : (b + 1) * LANES]
            turned.append(jnp.concatenate([ar * c + ai * s, ai * c - ar * s], axis=1))
        t = jnp.concatenate(turned, axis=0)
        hi = t.astype(bf16)
        lo = (t - hi.astype(f32)).astype(bf16)
        spec = dot(hi, cols_ref[0]) + dot(hi, cols_ref[1]) + dot(lo, cols_ref[0])
        spec_ref[...] = spec.reshape(spec_ref.shape)


def make_spectrum(length, filter_in, filter_mid, out_cut, rate_cut, tables):
    real_rows, _, _, fore_cols, _, turn = tables
    narrow = rate_cut.shape[0]
    bands = (filter_in.shape[0] - 1) // 2
    units = filter_mid.shape[0]
    sigs = 2 * narrow
    pad_rows = -(-filter_in.shape[0] // 8) * 8
    w_in = jnp.pad(filter_in.T, ((0, 0), (0, pad_rows - filter_in.shape[0])))
    w_mid = filter_mid.T
    w_out = out_cut.transpose(1, 2, 3, 0).reshape(2, sigs, units)
    rates = jnp.broadcast_to(rate_cut[:, None], (narrow, LANES))
    full = 2 * length
    chunk = 2048
    steps = full // chunk
    sig_batch = min(4, sigs)
    rows = full // LANES
    whole = lambda shape: pl.BlockSpec(shape, lambda i: (0,) * len(shape))
    return pl.pallas_call(
        functools.partial(filter_kernel, bands, length, sig_batch, chunk, steps),
        grid=(steps + sigs // sig_batch,),
        in_specs=[
            whole(w_in.shape),
            whole(w_mid.shape),
            whole(w_out.shape),
            whole(rates.shape),
            whole(real_rows.shape),
            whole(fore_cols.shape),
            whole(turn.shape),
        ],
        out_specs=pl.BlockSpec(
            (sig_batch, rows, 2 * LANES), lambda i: (jnp.maximum(i - steps, 0), 0, 0)
        ),
        out_shape=jax.ShapeDtypeStruct((sigs, rows, 2 * LANES), f32),
        scratch_shapes=[
            pltpu.VMEM((rows * sigs, LANES), f32),
            pltpu.VMEM((sigs, LANES), f32),
        ],
        compiler_params=pltpu.CompilerParams(vmem_limit_bytes=56 * 2**20),
        cost_estimate=pl.CostEstimate(
            flops=30_000_000_000, bytes_accessed=sigs * rows * 1024, transcendentals=0
        ),
        name="filter_spectrum",
    )(w_in, w_mid, w_out, rates, real_rows, fore_cols, turn)


def conv_kernel(
    batch, x_ref, taps, gain, spec_ref, pair_ref, unpair_ref, fore_ref, back_ref, turn_ref,
    out0, out1, held, done
):
    i = pl.program_id(0)
    groups, pieces, narrow, tok_rows = x_ref.shape
    tiles = tok_rows // LANES
    rows = turn_ref.shape[1]

    @pl.when(i == 0)
    def _():
        lane = lax.broadcasted_iota(jnp.int32, (narrow, LANES), 1)
        for p in range(3):
            before, mid, after = taps[p], taps[3 + p], taps[6 + p]
            for s in range(2):
                ps = 2 * p + s

                def step(r, carry):
                    last = x_ref[jnp.maximum(r - 1, 0), ps, :, tok_rows - LANES :].astype(f32)
                    follow = x_ref[jnp.minimum(r + 1, groups - 1), ps, :, :LANES].astype(f32)
                    span = [last * jnp.where(r > 0, 1.0, 0.0)]
                    for j in range(tiles):
                        span.append(x_ref[r, ps, :, j * LANES : (j + 1) * LANES].astype(f32))
                    span.append(follow * jnp.where(r < groups - 1, 1.0, 0.0))
                    up = [pltpu.roll(v, 1, 1) for v in span[:-1]]
                    down = [pltpu.roll(v, LANES - 1, 1) for v in span[1:]]
                    for j in range(tiles):
                        prev = jnp.where(lane == 0, up[j], up[j + 1])
                        nxt = jnp.where(lane == LANES - 1, down[j + 1], down[j])
                        at = ((ps * groups + r) * tiles + j) * narrow
                        held[pl.ds(at, narrow), :] = before * prev + mid * span[j + 1] + after * nxt
                    return carry

                lax.fori_loop(0, groups, step, 0)

    c, s = turn_ref[0], turn_ref[1]
    first = i * batch

    def part(p, b):
        return held[pl.ds(p * rows * narrow + first + b, rows, stride=narrow), :]

    def lanes(v, b):
        return v[:, b * LANES : (b + 1) * LANES]

    carried = [part(0, b) for b in range(batch)]
    for o in range(2):
        z = jnp.concatenate([v.astype(bf16) for v in carried], axis=1)
        a = dot(pair_ref[0], z) + dot(pair_ref[1], z)
        turned = []
        for b in range(batch):
            ar, ai = lanes(a[:rows], b), lanes(a[rows:], b)
            turned.append(
                jnp.concatenate([(ar * c + ai * s).astype(bf16), (ai * c - ar * s).astype(bf16)], axis=1)
            )
        t = jnp.concatenate(turned, axis=0)
        spec = dot(t, fore_ref[0]) + dot(t, fore_ref[1])
        prods = []
        for b in range(batch):
            sr = spec[b * rows : (b + 1) * rows, :LANES]
            si = spec[b * rows : (b + 1) * rows, LANES:]
            kr = spec_ref[o, b, :, :LANES]
            ki = spec_ref[o, b, :, LANES:]
            prods.append(
                jnp.concatenate([(sr * kr - si * ki).astype(bf16), (sr * ki + si * kr).astype(bf16)], axis=1)
            )
        t = jnp.concatenate(prods, axis=0)
        g = dot(t, back_ref[0]) + dot(t, back_ref[1])
        turned = []
        for b in range(batch):
            gr = g[b * rows : (b + 1) * rows, :LANES]
            gi = g[b * rows : (b + 1) * rows, LANES:]
            turned.append(
                jnp.concatenate([(gr * c - gi * s).astype(bf16), (gi * c + gr * s).astype(bf16)], axis=0)
            )
        h = jnp.concatenate(turned, axis=1)
        y = dot(unpair_ref[0], h) + dot(unpair_ref[1], h)
        carried = [
            part(o + 1, b) * (lanes(y, b) + gain[o, first + b] * carried[b]) for b in range(batch)
        ]
    for b in range(batch):
        done[pl.ds(first + b, rows, stride=narrow), :] = carried[b]

    @pl.when(i == pl.num_programs(0) - 1)
    def _():
        for s_idx, out in enumerate((out0, out1)):

            def leave(r, carry):
                for j in range(tiles):
                    at = ((s_idx * groups + r) * tiles + j) * narrow
                    out[r, :, j * LANES : (j + 1) * LANES] = done[pl.ds(at, narrow), :].astype(bf16)
                return carry

            lax.fori_loop(0, groups, leave, 0)


def gated_conv(arrived, tap_cut, gain_cut, spectrum, tables):
    _, pair_rows, unpair_rows, fore_cols, back_cols, turn = tables
    groups, _, narrow, tok_rows = arrived.shape
    rows = turn.shape[1]
    batch = min(4, narrow)
    taps = jnp.broadcast_to(tap_cut.reshape(9, narrow)[:, :, None], (9, narrow, LANES))
    spectrum = spectrum.reshape(2, narrow, rows, 2 * LANES)
    whole = lambda shape: pl.BlockSpec(shape, lambda i: (0,) * len(shape))
    out = jax.ShapeDtypeStruct((groups, narrow, tok_rows), bf16)
    return pl.pallas_call(
        functools.partial(conv_kernel, batch),
        grid=(narrow // batch,),
        in_specs=[
            whole(arrived.shape),
            whole(taps.shape),
            pl.BlockSpec(memory_space=pltpu.SMEM),
            pl.BlockSpec((2, batch, rows, 2 * LANES), lambda i: (0, i, 0, 0)),
            whole(pair_rows.shape),
            whole(unpair_rows.shape),
            whole(fore_cols.shape),
            whole(back_cols.shape),
            whole(turn.shape),
        ],
        out_specs=[whole(out.shape), whole(out.shape)],
        out_shape=[out, out],
        scratch_shapes=[
            pltpu.VMEM((3 * rows * narrow, LANES), f32),
            pltpu.VMEM((rows * narrow, LANES), f32),
        ],
        compiler_params=pltpu.CompilerParams(vmem_limit_bytes=56 * 2**20),
        cost_estimate=pl.CostEstimate(
            flops=20_000_000_000, bytes_accessed=narrow * rows * 2048, transcendentals=0
        ),
        name="gated_conv",
    )(arrived, taps, gain_cut, spectrum, pair_rows, unpair_rows, fore_cols, back_cols, turn)


def on_device(
    tokens,
    w_value,
    w_first,
    w_second,
    short_taps,
    filter_in,
    filter_mid,
    filter_out,
    decay_rate,
    skip_gain,
    w_output,
):
    seq_count, tok_rows, _ = tokens.shape
    local_width = w_value.shape[1]
    groups = lax.axis_size("row")
    narrow = local_width // groups
    length = tok_rows * groups
    offset = lax.axis_index("row") * narrow
    tables = transform_tables(2 * length)
    projected = jnp.stack(
        [
            jnp.einsum("std,dc->sct", tokens, weight, preferred_element_type=f32).astype(bf16)
            for weight in (w_value, w_first, w_second)
        ]
    )
    projected = projected.reshape(3 * seq_count, groups, narrow, tok_rows).transpose(1, 0, 2, 3)
    arrived = lax.all_to_all(projected, "row", split_axis=0, concat_axis=0, tiled=True)
    tap_cut = lax.dynamic_slice_in_dim(short_taps, offset, narrow, 2)
    rate_cut = lax.dynamic_slice_in_dim(decay_rate, offset, narrow, 0)
    gain_cut = lax.dynamic_slice_in_dim(skip_gain, offset, narrow, 1)
    out_cut = lax.dynamic_slice_in_dim(filter_out, offset, narrow, 3)
    spectrum = make_spectrum(length, filter_in, filter_mid, out_cut, rate_cut, tables)
    gated = gated_conv(arrived, tap_cut, gain_cut, spectrum, tables)
    results = []
    for piece in gated:
        returned = lax.all_to_all(piece, "row", split_axis=0, concat_axis=0, tiled=True)
        returned = returned.reshape(local_width, tok_rows)
        gathered = lax.all_gather(returned, "col", axis=0, tiled=True)
        results.append(
            jnp.einsum("ct,cd->td", gathered, w_output, preferred_element_type=f32).astype(bf16)
        )
    return jnp.stack(results)


def solution(mesh):
    placed = (
        P(None, "row", None),
        P(None, "col"),
        P(None, "col"),
        P(None, "col"),
        P(None, None, "col"),
        P(),
        P(),
        P(None, None, None, "col"),
        P("col"),
        P(None, "col"),
        P(None, "col"),
    )
    return jax.shard_map(
        on_device, mesh=mesh, in_specs=placed, out_specs=P(None, "row", "col"), check_vma=False
    )
```

```python
import functools
import math

import jax
import jax.numpy as jnp
import numpy as np
from jax import lax
from jax.experimental import pallas as pl
from jax.experimental.pallas import tpu as pltpu
from jax.sharding import PartitionSpec as P

LANES = 128
f32 = jnp.float32
bf16 = jnp.bfloat16
highest = lax.Precision.HIGHEST


def split_table(table):
    table = np.asarray(table, np.float32)
    high = table.astype(bf16)
    low = (table - high.astype(np.float32)).astype(bf16)
    return np.stack([high, low])


def transform_tables(full_length):
    rows = full_length // LANES
    half = rows // 2
    r = np.arange(rows)
    q = np.arange(LANES)
    angle_rows = 2.0 * np.pi * ((r[:, None] * r[None, :]) % rows) / rows
    angle_cols = 2.0 * np.pi * ((q[:, None] * q[None, :]) % LANES) / LANES
    angle_turn = 2.0 * np.pi * ((r[:, None] * q[None, :]) % full_length) / full_length
    c1, s1 = np.cos(angle_rows), np.sin(angle_rows)
    c2, s2 = np.cos(angle_cols), np.sin(angle_cols)
    real_rows = split_table(np.concatenate([c1, -s1], 0))
    pair_rows = np.block([[c1[:, :half], s1[:, :half]], [-s1[:, :half], c1[:, :half]]])
    fore_cols = np.block([[c2, -s2], [s2, c2]])
    back_cols = np.block([[c2, s2], [-s2, c2]])
    turn = np.stack([np.cos(angle_turn), np.sin(angle_turn)]).astype(np.float32)
    return (
        real_rows,
        split_table(pair_rows),
        split_table(pair_rows.T),
        split_table(fore_cols),
        split_table(back_cols),
        turn,
    )


def dot(a, b):
    return jnp.dot(a, b, preferred_element_type=f32)


def wave(x):
    turns = jnp.floor(x * (1.0 / math.pi) + 0.5)
    r = x - turns * 3.140625
    r = r - turns * 9.67502593994140625e-4
    r = r - turns * 1.509957990978376e-7
    odd = turns - 2.0 * jnp.floor(turns * 0.5)
    r = r * (1.0 - 2.0 * odd)
    q = r * r
    p = -2.5052108e-8
    for coef in (2.7557319e-6, -1.9841270e-4, 8.3333333e-3, -1.6666667e-1):
        p = p * q + coef
    return r + r * q * p


def filter_kernel(
    bands, length, sig_batch, chunk, steps, w_in, w_mid, w_out, rates, rows_ref, cols_ref, turn_ref,
    spec_ref, line_ref, power_ref
):
    i = pl.program_id(0)
    sigs = w_out.shape[1]
    full = 2 * length
    n1_count = full // LANES

    @pl.when(i == 0)
    def _():
        power_ref[...] = jnp.zeros_like(power_ref)

    @pl.when(i < steps)
    def _():
        feat_rows = w_in.shape[1]
        n = i * chunk + lax.broadcasted_iota(jnp.int32, (1, chunk), 1)
        m = jnp.where(n < length, n, full - n).astype(f32)
        row = lax.broadcasted_iota(jnp.int32, (feat_rows, 1), 0)
        band = jnp.where(row <= bands, row - 1, row - 1 - bands).astype(f32)
        freq = 0.0001 + (bands - 1 - 0.0001) / (bands - 1) * band
        phase = jnp.where(row <= bands, 0.5 * math.pi, math.pi).astype(f32)
        angle = (2.0 * math.pi / length * m) * freq + phase
        feats = jnp.where(
            row == 0, m * (1.0 / (length - 1)), jnp.where(row <= 2 * bands, wave(angle), 0.0)
        )
        hidden = wave(jnp.dot(w_in[...], feats, precision=highest, preferred_element_type=f32))
        hidden = wave(jnp.dot(w_mid[...], hidden, precision=highest, preferred_element_type=f32))
        side = i // (steps // 2)
        shaped = jnp.dot(w_out[side], hidden, precision=highest, preferred_element_type=f32)
        damp = jnp.exp(-rates[:, 0:1] * m)
        damp = jnp.where(n == length, 0.0, damp)
        shaped = shaped * jnp.concatenate([damp, damp], axis=0)
        power = power_ref[...]
        for j in range(chunk // LANES):
            tile = shaped[:, j * LANES : (j + 1) * LANES]
            power = power + tile * tile
            at = pl.multiple_of((i * (chunk // LANES) + j) * sigs, sigs)
            line_ref[pl.ds(at, sigs), :] = tile
        power_ref[...] = power

    @pl.when(i == steps)
    def _():
        total = jnp.sum(power_ref[...], axis=1, keepdims=True)
        power_ref[...] = jnp.broadcast_to(lax.rsqrt(total + 1e-6) * (1.0 / full), power_ref.shape)

    @pl.when(i >= steps)
    def _():
        c, s = turn_ref[0], turn_ref[1]
        first = (i - steps) * sig_batch
        parts = []
        for b in range(sig_batch):
            line = line_ref[pl.ds(first + b, n1_count, stride=sigs), :]
            parts.append(line * power_ref[pl.ds(first + b, 1), :])
        x = jnp.concatenate(parts, axis=1)
        hi = x.astype(bf16)
        lo = (x - hi.astype(f32)).astype(bf16)
        a = dot(rows_ref[0], hi) + dot(rows_ref[1], hi) + dot(rows_ref[0], lo)
        turned = []
        for b in range(sig_batch):
            ar = a[:n1_count, b * LANES : (b + 1) * LANES]
            ai = a[n1_count:, b * LANES : (b + 1) * LANES]
            turned.append(jnp.concatenate([ar * c + ai * s, ai * c - ar * s], axis=1))
        t = jnp.concatenate(turned, axis=0)
        hi = t.astype(bf16)
        lo = (t - hi.astype(f32)).astype(bf16)
        spec = dot(hi, cols_ref[0]) + dot(hi, cols_ref[1]) + dot(lo, cols_ref[0])
        spec_ref[...] = spec.reshape(spec_ref.shape)


def make_spectrum(length, filter_in, filter_mid, out_cut, rate_cut, tables):
    real_rows, _, _, fore_cols, _, turn = tables
    narrow = rate_cut.shape[0]
    bands = (filter_in.shape[0] - 1) // 2
    units = filter_mid.shape[0]
    sigs = 2 * narrow
    pad_rows = -(-filter_in.shape[0] // 8) * 8
    w_in = jnp.pad(filter_in.T, ((0, 0), (0, pad_rows - filter_in.shape[0])))
    w_mid = filter_mid.T
    w_out = out_cut.transpose(1, 2, 3, 0).reshape(2, sigs, units)
    rates = jnp.broadcast_to(rate_cut[:, None], (narrow, LANES))
    full = 2 * length
    chunk = 2048
    steps = full // chunk
    sig_batch = min(4, sigs)
    rows = full // LANES
    whole = lambda shape: pl.BlockSpec(shape, lambda i: (0,) * len(shape))
    return pl.pallas_call(
        functools.partial(filter_kernel, bands, length, sig_batch, chunk, steps),
        grid=(steps + sigs // sig_batch,),
        in_specs=[
            whole(w_in.shape),
            whole(w_mid.shape),
            whole(w_out.shape),
            whole(rates.shape),
            whole(real_rows.shape),
            whole(fore_cols.shape),
            whole(turn.shape),
        ],
        out_specs=pl.BlockSpec(
            (sig_batch, rows, 2 * LANES), lambda i: (jnp.maximum(i - steps, 0), 0, 0)
        ),
        out_shape=jax.ShapeDtypeStruct((sigs, rows, 2 * LANES), f32),
        scratch_shapes=[
            pltpu.VMEM((rows * sigs, LANES), f32),
            pltpu.VMEM((sigs, LANES), f32),
        ],
        compiler_params=pltpu.CompilerParams(vmem_limit_bytes=56 * 2**20),
        cost_estimate=pl.CostEstimate(
            flops=30_000_000_000, bytes_accessed=sigs * rows * 1024, transcendentals=0
        ),
        name="filter_spectrum",
    )(w_in, w_mid, w_out, rates, real_rows, fore_cols, turn)


def conv_kernel(
    batch, x_ref, taps, gain, spec_ref, pair_ref, unpair_ref, fore_ref, back_ref, turn_ref,
    out, held, done
):
    i = pl.program_id(0)
    groups, pieces, narrow, tok_rows = x_ref.shape
    tiles = tok_rows // LANES
    rows = turn_ref.shape[1]

    @pl.when(i == 0)
    def _():
        lane = lax.broadcasted_iota(jnp.int32, (narrow, LANES), 1)
        for p in range(3):
            before, mid, after = taps[p], taps[3 + p], taps[6 + p]
            for s in range(2):
                ps = 2 * p + s

                def step(r, carry):
                    last = x_ref[jnp.maximum(r - 1, 0), ps, :, tok_rows - LANES :].astype(f32)
                    follow = x_ref[jnp.minimum(r + 1, groups - 1), ps, :, :LANES].astype(f32)
                    span = [last * jnp.where(r > 0, 1.0, 0.0)]
                    for j in range(tiles):
                        span.append(x_ref[r, ps, :, j * LANES : (j + 1) * LANES].astype(f32))
                    span.append(follow * jnp.where(r < groups - 1, 1.0, 0.0))
                    up = [pltpu.roll(v, 1, 1) for v in span[:-1]]
                    down = [pltpu.roll(v, LANES - 1, 1) for v in span[1:]]
                    for j in range(tiles):
                        prev = jnp.where(lane == 0, up[j], up[j + 1])
                        nxt = jnp.where(lane == LANES - 1, down[j + 1], down[j])
                        at = ((ps * groups + r) * tiles + j) * narrow
                        held[pl.ds(at, narrow), :] = before * prev + mid * span[j + 1] + after * nxt
                    return carry

                lax.fori_loop(0, groups, step, 0)

    c, s = turn_ref[0], turn_ref[1]
    first = i * batch

    def part(p, b):
        return held[pl.ds(p * rows * narrow + first + b, rows, stride=narrow), :]

    def lanes(v, b):
        return v[:, b * LANES : (b + 1) * LANES]

    carried = [part(0, b) for b in range(batch)]
    for o in range(2):
        z = jnp.concatenate([v.astype(bf16) for v in carried], axis=1)
        a = dot(pair_ref[0], z) + dot(pair_ref[1], z)
        turned = []
        for b in range(batch):
            ar, ai = lanes(a[:rows], b), lanes(a[rows:], b)
            turned.append(
                jnp.concatenate([(ar * c + ai * s).astype(bf16), (ai * c - ar * s).astype(bf16)], axis=1)
            )
        t = jnp.concatenate(turned, axis=0)
        spec = dot(t, fore_ref[0]) + dot(t, fore_ref[1])
        prods = []
        for b in range(batch):
            sr = spec[b * rows : (b + 1) * rows, :LANES]
            si = spec[b * rows : (b + 1) * rows, LANES:]
            kr = spec_ref[o, b, :, :LANES]
            ki = spec_ref[o, b, :, LANES:]
            prods.append(
                jnp.concatenate([(sr * kr - si * ki).astype(bf16), (sr * ki + si * kr).astype(bf16)], axis=1)
            )
        t = jnp.concatenate(prods, axis=0)
        g = dot(t, back_ref[0]) + dot(t, back_ref[1])
        turned = []
        for b in range(batch):
            gr = g[b * rows : (b + 1) * rows, :LANES]
            gi = g[b * rows : (b + 1) * rows, LANES:]
            turned.append(
                jnp.concatenate([(gr * c - gi * s).astype(bf16), (gi * c + gr * s).astype(bf16)], axis=0)
            )
        h = jnp.concatenate(turned, axis=1)
        y = dot(unpair_ref[0], h) + dot(unpair_ref[1], h)
        carried = [
            part(o + 1, b) * (lanes(y, b) + gain[o, first + b] * carried[b]) for b in range(batch)
        ]
    for b in range(batch):
        done[pl.ds(first + b, rows, stride=narrow), :] = carried[b]

    @pl.when(i == pl.num_programs(0) - 1)
    def _():
        for s_idx in range(2):

            def leave(r, carry):
                for j in range(tiles):
                    at = ((s_idx * groups + r) * tiles + j) * narrow
                    out[r, s_idx, :, j * LANES : (j + 1) * LANES] = done[pl.ds(at, narrow), :].astype(bf16)
                return carry

            lax.fori_loop(0, groups, leave, 0)


def gated_conv(arrived, tap_cut, gain_cut, spectrum, tables):
    _, pair_rows, unpair_rows, fore_cols, back_cols, turn = tables
    groups, _, narrow, tok_rows = arrived.shape
    rows = turn.shape[1]
    batch = min(4, narrow)
    taps = jnp.broadcast_to(tap_cut.reshape(9, narrow)[:, :, None], (9, narrow, LANES))
    spectrum = spectrum.reshape(2, narrow, rows, 2 * LANES)
    whole = lambda shape: pl.BlockSpec(shape, lambda i: (0,) * len(shape))
    out = jax.ShapeDtypeStruct((groups, 2, narrow, tok_rows), bf16)
    return pl.pallas_call(
        functools.partial(conv_kernel, batch),
        grid=(narrow // batch,),
        in_specs=[
            whole(arrived.shape),
            whole(taps.shape),
            pl.BlockSpec(memory_space=pltpu.SMEM),
            pl.BlockSpec((2, batch, rows, 2 * LANES), lambda i: (0, i, 0, 0)),
            whole(pair_rows.shape),
            whole(unpair_rows.shape),
            whole(fore_cols.shape),
            whole(back_cols.shape),
            whole(turn.shape),
        ],
        out_specs=whole(out.shape),
        out_shape=out,
        scratch_shapes=[
            pltpu.VMEM((3 * rows * narrow, LANES), f32),
            pltpu.VMEM((rows * narrow, LANES), f32),
        ],
        compiler_params=pltpu.CompilerParams(vmem_limit_bytes=56 * 2**20),
        cost_estimate=pl.CostEstimate(
            flops=20_000_000_000, bytes_accessed=narrow * rows * 2048, transcendentals=0
        ),
        name="gated_conv",
    )(arrived, taps, gain_cut, spectrum, pair_rows, unpair_rows, fore_cols, back_cols, turn)


def return_kernel(groups, x, out, own, own_sem, send_sem, recv_sem, pass_sem, take_sem):
    me = lax.axis_index("row")
    side = lax.axis_index("col")
    mesh_ids = pl.DeviceIdType.MESH
    barrier = pltpu.get_barrier_semaphore()
    for k in range(1, groups):
        peer = lax.rem(me + k, groups)
        pl.semaphore_signal(barrier, inc=1, device_id=(peer, side), device_id_type=mesh_ids)
    pl.semaphore_signal(barrier, inc=1, device_id=(me, 1 - side), device_id_type=mesh_ids)
    pl.semaphore_wait(barrier, groups)

    sends = []
    for k in range(1, groups):
        peer = lax.rem(me + k, groups)
        sends.append(
            pltpu.make_async_remote_copy(
                src_ref=x.at[peer],
                dst_ref=out.at[:, side, me],
                send_sem=send_sem.at[k],
                recv_sem=recv_sem.at[k],
                device_id=(peer, side),
                device_id_type=mesh_ids,
            )
        )
        sends[-1].start()

    def hand_over(k, source, place):
        copy = pltpu.make_async_remote_copy(
            src_ref=source,
            dst_ref=out.at[:, side, place],
            send_sem=pass_sem.at[k],
            recv_sem=take_sem.at[k],
            device_id=(me, 1 - side),
            device_id_type=mesh_ids,
        )
        copy.start()
        return copy

    passes = [hand_over(0, x.at[me], me)]
    fetch = pltpu.make_async_copy(x.at[me], own, own_sem.at[0])
    fetch.start()
    fetch.wait()
    keep = pltpu.make_async_copy(own, out.at[:, side, me], own_sem.at[1])
    keep.start()
    for k in range(1, groups):
        sends[k - 1].wait_recv()
        source = lax.rem(me + groups - k, groups)
        passes.append(hand_over(k, out.at[:, side, source], source))
    keep.wait()
    for copy in sends:
        copy.wait_send()
    for copy in passes:
        copy.wait()


def return_blocks(gated):
    groups, seqs, narrow, tok_rows = gated.shape
    out = pl.pallas_call(
        functools.partial(return_kernel, groups),
        in_specs=[pl.BlockSpec(memory_space=pl.ANY)],
        out_specs=pl.BlockSpec(memory_space=pl.ANY),
        out_shape=jax.ShapeDtypeStruct((seqs, 2, groups, narrow, tok_rows), bf16),
        scratch_shapes=[
            pltpu.VMEM((seqs, narrow, tok_rows), bf16),
            pltpu.SemaphoreType.DMA((2,)),
            pltpu.SemaphoreType.DMA((groups,)),
            pltpu.SemaphoreType.DMA((groups,)),
            pltpu.SemaphoreType.DMA((groups,)),
            pltpu.SemaphoreType.DMA((groups,)),
        ],
        compiler_params=pltpu.CompilerParams(collective_id=0, has_side_effects=True),
        name="return_blocks",
    )(gated)
    return out.reshape(seqs, 2 * groups * narrow, tok_rows)


def on_device(
    tokens,
    w_value,
    w_first,
    w_second,
    short_taps,
    filter_in,
    filter_mid,
    filter_out,
    decay_rate,
    skip_gain,
    w_output,
):
    seq_count, tok_rows, _ = tokens.shape
    local_width = w_value.shape[1]
    groups = lax.axis_size("row")
    narrow = local_width // groups
    length = tok_rows * groups
    offset = lax.axis_index("row") * narrow
    tables = transform_tables(2 * length)
    projected = jnp.stack(
        [
            jnp.einsum("std,dc->sct", tokens, weight, preferred_element_type=f32).astype(bf16)
            for weight in (w_value, w_first, w_second)
        ]
    )
    projected = projected.reshape(3 * seq_count, groups, narrow, tok_rows).transpose(1, 0, 2, 3)
    arrived = lax.all_to_all(projected, "row", split_axis=0, concat_axis=0, tiled=True)
    tap_cut = lax.dynamic_slice_in_dim(short_taps, offset, narrow, 2)
    rate_cut = lax.dynamic_slice_in_dim(decay_rate, offset, narrow, 0)
    gain_cut = lax.dynamic_slice_in_dim(skip_gain, offset, narrow, 1)
    out_cut = lax.dynamic_slice_in_dim(filter_out, offset, narrow, 3)
    spectrum = make_spectrum(length, filter_in, filter_mid, out_cut, rate_cut, tables)
    gated = gated_conv(arrived, tap_cut, gain_cut, spectrum, tables)
    if groups <= 16 and lax.axis_size("col") == 2:
        gathered = return_blocks(gated)
    else:
        returned = lax.all_to_all(gated, "row", split_axis=0, concat_axis=0, tiled=True)
        returned = returned.transpose(1, 0, 2, 3).reshape(seq_count, local_width, tok_rows)
        gathered = lax.all_gather(returned, "col", axis=1, tiled=True)
    result = jnp.einsum("sct,cd->std", gathered, w_output, preferred_element_type=f32)
    return result.astype(bf16)


def solution(mesh):
    placed = (
        P(None, "row", None),
        P(None, "col"),
        P(None, "col"),
        P(None, "col"),
        P(None, None, "col"),
        P(),
        P(),
        P(None, None, None, "col"),
        P("col"),
        P(None, "col"),
        P(None, "col"),
    )
    return jax.shard_map(
        on_device, mesh=mesh, in_specs=placed, out_specs=P(None, "row", "col"), check_vma=False
    )
```
